32 devices in a mesh: sp: 8 (over z, y), tp: 4 (over x, core).
Axes of the slice: x: 2, y: 2, z: 4, core: 2. Of those that a mesh axis runs over, the one named last changes fastest.
Arguments:
- queries: bfloat16 [1, 2048, 2048], P(None, 'sp', 'tp'), may hold values from -5 to 5
- key_vectors: bfloat16 [1, 2048, 2048], P(None, 'sp', 'tp'), may hold values from -5 to 5
- value_vectors: bfloat16 [1, 2048, 2048], P(None, 'sp', 'tp'), may hold values from -40 to 40
- cotangent: bfloat16 [1, 2048, 2048], P(None, 'sp', 'tp'), may hold values from -6 to 6
- out_gain: bfloat16 [2048], P('tp'), may hold values from 0.099609375 to 1.8984375
- rel_table: bfloat16 [16, 320], P('tp'), may hold values from -4 to 4
Outputs:
- grad_queries: bfloat16 [1, 2048, 2048], P(None, 'sp', 'tp')
- grad_keys: bfloat16 [1, 2048, 2048], P(None, 'sp', 'tp')
- grad_values: bfloat16 [1, 2048, 2048], P(None, 'sp', 'tp')
- grad_table: float32 [16, 320], P('tp')
The draws below stay inside these ranges and needn't reach their ends.
All inputs are finite; a program needn't handle non-finite values.
Results may differ from the reference program's by a relative error of at most 0.0071.
Values may be sent and summed in bfloat16 or wider, within the bound.
A program may use at most 64 MiB of HBM per device.

```python
import math
import jax
import jax.numpy as jnp
import numpy as np
from jax import lax

HEADS = 16
HEAD_DIM = 128
SEG = 64
LEFT = 4
MAX_REL = 256
SEQS = 1
WIDTH = 2048
REL = 320
TOKENS = 2048


def head_scale():
    head_ids = (jnp.arange(WIDTH) // HEAD_DIM).astype(jnp.float32)
    return 3.0 ** (head_ids / (HEADS - 1))


def normal_rows(key, salt):
    normal_part = jax.random.normal(jax.random.fold_in(key, salt), (SEQS, TOKENS, WIDTH), jnp.float32)
    return jnp.clip(normal_part, -5.0, 5.0).reshape(SEQS, TOKENS // SEG, SEG, WIDTH)


def draw_queries(key, part):
    rows_out = normal_rows(key, 1)
    return rows_out.reshape(SEQS, TOKENS, WIDTH).astype(jnp.bfloat16)


def draw_key_vectors(key, part):
    rows_out = normal_rows(key, 2)
    return rows_out.reshape(SEQS, TOKENS, WIDTH).astype(jnp.bfloat16)


def draw_value_vectors(key, part):
    base_key = jax.random.fold_in(jax.random.fold_in(key, 3), 0)
    body_part = jnp.clip(jax.random.normal(base_key, (SEQS, TOKENS, WIDTH), jnp.float32), -4.0, 4.0)
    return (body_part * head_scale()).astype(jnp.bfloat16)


def block_levels(stream_key, extent, cuts, low, high):
    def one(position, blocks):
        draws = jax.random.uniform(jax.random.fold_in(jax.random.fold_in(stream_key, 6), position), (blocks,), jnp.float32, low / len(cuts), high / len(cuts))
        return jnp.repeat(jnp.exp(draws), extent[position] // blocks).reshape((-1,) + (1,) * (len(extent) - position - 1))

    factor_of = one(*cuts[0])
    for cut in cuts[1:]:
        factor_of = factor_of * one(*cut)
    return factor_of


def scatter_about(key, shape, spread, bound, shards=(), dtype=jnp.bfloat16):
    result = spread * jax.random.normal(key, shape, jnp.float32)
    if shards:
        result = result * block_levels(key, shape, shards, -0.22, 0.18)
    return jnp.clip(result, -bound, bound).astype(dtype)


def setup_inputs(seed: int = 0) -> dict:
    key_list = jax.random.split(jax.random.key(seed), 7)
    queries = draw_queries(jax.random.fold_in(key_list[6], 71), 0)
    key_vectors = draw_key_vectors(jax.random.fold_in(key_list[6], 71), 0)
    value_vectors = draw_value_vectors(jax.random.fold_in(key_list[6], 71), 0)
    cotangent = scatter_about(key_list[3], (SEQS, TOKENS, WIDTH), 1.0, 6.0, ((1, 8), (2, 4)))
    out_gain = jnp.clip(1.0 + 0.18 * jax.random.normal(key_list[4], (WIDTH,), jnp.float32), 0.099609375, 1.8984375).astype(jnp.bfloat16)
    rel_table = scatter_about(key_list[5], (HEADS, REL), 1.0, 4.0, ((0, 4),))
    return dict(queries=queries, key_vectors=key_vectors, value_vectors=value_vectors, cotangent=cotangent, out_gain=out_gain, rel_table=rel_table)


epsilon = 1e-06
masked_value = -1e+30

def band_index():
    query_pos = np.arange(SEG)[:, None, None]
    band_pos = np.arange(LEFT + 1)[None, :, None]
    key_pos = np.arange(SEG)[None, None, :]
    distance = (LEFT - band_pos) * SEG + query_pos - key_pos
    return (np.minimum(distance, MAX_REL) + SEG - 1).astype(np.int32)

def expand_bias(table_rows):
    return jnp.take(table_rows, jnp.asarray(band_index()), axis=1)

def padded_segments(rows_in):
    padded = jnp.pad(rows_in.astype(jnp.float32), ((LEFT * SEG, 0), (0, 0)))
    return padded.reshape(-1, SEG, HEAD_DIM)

def lowered(array):
    rounded = lax.optimization_barrier(array.astype(jnp.bfloat16))
    return rounded.astype(jnp.float32)

def head_probs(query_seg, key_pad, pos_bias, seg_count):
    scores = jnp.stack([jnp.einsum('cqd,ckd->cqk', query_seg, key_pad[offset:offset + seg_count]) for offset in range(LEFT + 1)], axis=2)
    scores = scores / math.sqrt(HEAD_DIM) + pos_bias[None]
    visible = np.arange(seg_count)[:, None] - LEFT + np.arange(LEFT + 1)[None, :] >= 0
    scores = jnp.where(visible[:, None, :, None], scores, masked_value)
    flat = jax.nn.softmax(scores.reshape(seg_count, SEG, -1), axis=-1)
    return flat.reshape(scores.shape)

def forward_head(packed):
    query_rows, key_rows, value_rows, pos_bias = packed
    seg_count = query_rows.shape[0] // SEG
    query_seg = query_rows.astype(jnp.float32).reshape(seg_count, SEG, HEAD_DIM)
    probability = head_probs(query_seg, padded_segments(key_rows), pos_bias, seg_count)
    prob_low = lowered(probability)
    value_pad = padded_segments(value_rows)
    attended = sum((jnp.einsum('cqk,ckd->cqd', prob_low[:, :, offset], value_pad[offset:offset + seg_count]) for offset in range(LEFT + 1)))
    return attended.reshape(-1, HEAD_DIM)

def backward_head(packed):
    query_rows, key_rows, value_rows, grad_rows, pos_bias = packed
    seg_count = query_rows.shape[0] // SEG
    query_seg = query_rows.astype(jnp.float32).reshape(seg_count, SEG, HEAD_DIM)
    key_pad = padded_segments(key_rows)
    value_pad = padded_segments(value_rows)
    probability = head_probs(query_seg, key_pad, pos_bias, seg_count)
    prob_low = lowered(probability)
    grad_seg = grad_rows.astype(jnp.float32).reshape(seg_count, SEG, HEAD_DIM)
    grad_probs = jnp.stack([jnp.einsum('cqd,ckd->cqk', grad_seg, value_pad[offset:offset + seg_count]) for offset in range(LEFT + 1)], axis=2)
    row_dot = lax.optimization_barrier(jnp.sum(probability * grad_probs, axis=(2, 3), keepdims=True))
    grad_scores = probability * (grad_probs - row_dot)
    grad_low = lowered(grad_scores)
    scale_root = math.sqrt(HEAD_DIM)
    grad_query = sum((jnp.einsum('cqk,ckd->cqd', grad_low[:, :, offset], key_pad[offset:offset + seg_count]) for offset in range(LEFT + 1))) / scale_root
    key_grad = jnp.zeros((seg_count + LEFT, SEG, HEAD_DIM), jnp.float32)
    value_grad = jnp.zeros((seg_count + LEFT, SEG, HEAD_DIM), jnp.float32)
    for offset in range(LEFT + 1):
        key_grad = key_grad.at[offset:offset + seg_count].add(jnp.einsum('cqk,cqd->ckd', grad_low[:, :, offset], query_seg))
        value_grad = value_grad.at[offset:offset + seg_count].add(jnp.einsum('cqk,cqd->ckd', prob_low[:, :, offset], grad_seg))
    return (grad_query.reshape(-1, HEAD_DIM).astype(jnp.bfloat16), (key_grad[LEFT:] / scale_root).reshape(-1, HEAD_DIM).astype(jnp.bfloat16), value_grad[LEFT:].reshape(-1, HEAD_DIM).astype(jnp.bfloat16), lax.optimization_barrier(jnp.sum(grad_scores, axis=0)))

def split_heads(array):
    return array.reshape(array.shape[0], HEADS, HEAD_DIM).transpose(1, 0, 2)

def merge_heads(array):
    return array.transpose(1, 0, 2).reshape(array.shape[1], HEADS * HEAD_DIM)

def reference(queries, key_vectors, value_vectors, cotangent, out_gain, rel_table):
    pos_bias, pullback = jax.vjp(expand_bias, rel_table.astype(jnp.float32))
    gain_rows = out_gain.astype(jnp.float32)

    def one_sequence(packed):
        query_seq, key_seq, value_seq, cot_seq = packed
        query_heads = split_heads(query_seq)
        key_heads = split_heads(key_seq)
        value_heads = split_heads(value_seq)
        attended = merge_heads(lax.map(forward_head, (query_heads, key_heads, value_heads, pos_bias)))
        inv_rms = lax.rsqrt(lax.optimization_barrier(jnp.mean(attended * attended, axis=-1, keepdims=True)) + epsilon)
        scaled = cot_seq.astype(jnp.float32) * gain_rows
        mean_prod = lax.optimization_barrier(jnp.mean(attended * scaled, axis=-1, keepdims=True))
        grad_attended = (inv_rms * scaled - attended * inv_rms ** 3 * mean_prod).astype(jnp.bfloat16)
        grad_query, grad_key, grad_value, bias_grad = lax.map(backward_head, (query_heads, key_heads, value_heads, split_heads(grad_attended), pos_bias))
        return (merge_heads(grad_query), merge_heads(grad_key), merge_heads(grad_value), bias_grad)
    grad_queries, grad_keys, grad_values, bias_grads = lax.map(one_sequence, (queries, key_vectors, value_vectors, cotangent))
    grad_table = pullback(lax.optimization_barrier(jnp.sum(bias_grads, axis=0)))[0]
    return (grad_queries, grad_keys, grad_values, grad_table)
```

```python
import functools
import math

import jax
import jax.numpy as jnp
from jax import lax
from jax.experimental import pallas as pl
from jax.experimental.pallas import tpu as pltpu
from jax.sharding import PartitionSpec as P

HEAD_DIM = 128
SEG = 64
LEFT = 4
MAX_REL = 256
REACH = LEFT * SEG
ROWS = 2 * SEG
COLS = REACH + ROWS
ROLL = 512

epsilon = 1e-06
masked_value = -1e30
F32 = jnp.float32
BF16 = jnp.bfloat16
HIGHEST = lax.Precision.HIGHEST


def dot(left, right, left_dim, right_dim, precision=None):
    return lax.dot_general(
        left,
        right,
        (((left_dim,), (right_dim,)), ((), ())),
        preferred_element_type=F32,
        precision=precision,
    )


def iota(shape, dim):
    return lax.broadcasted_iota(jnp.int32, shape, dim)


def distance_picks(rel, columns, dim, offset):
    shape = (columns, ROLL) if dim == 0 else (ROLL, columns)
    column, lane = iota(shape, dim), (iota(shape, 1 - dim) + (ROLL - offset)) % ROLL
    wanted = jnp.minimum(rel - 1 - lane, rel - 1)
    inside = lane < rel
    wrapped = lane > ROLL - SEG
    hit = (inside & (column == wanted)) | (wrapped & (column == rel - 1))
    return jnp.where(hit, 1.0, 0.0).astype(BF16)


def in_parts(value):
    high = value.astype(BF16)
    rest = value - high.astype(F32)
    middle = rest.astype(BF16)
    low = (rest - middle.astype(F32)).astype(BF16)
    return jnp.concatenate([high, middle, low], axis=0)


def spread_rows(row):
    tile = jnp.broadcast_to(row, (8, ROLL))
    index = iota((8, ROLL), 0)
    for step in (1, 2, 4):
        tile = jnp.where((index & step) != 0, pltpu.roll(tile, step, 1), tile)
    step = 8
    while step < ROWS:
        tile = jnp.concatenate([tile, pltpu.roll(tile, step, 1)], axis=0)
        step *= 2
    return tile


def fold_rows(tile):
    total = tile[:8]
    for row in range(8, ROWS, 8):
        total = total + pltpu.roll(tile[row : row + 8], ROLL - row, 1)
    total = jnp.concatenate([total[row : row + 1] for row in reversed(range(8))], axis=0)
    return jnp.sum(pltpu.roll(total, 0, 1, stride=1, stride_axis=0), axis=0, keepdims=True)


def kernel(
    sp_count,
    tp_count,
    q_hbm,
    k_hbm,
    v_hbm,
    cot_hbm,
    gain_hbm,
    table_hbm,
    gq_ref,
    gk_ref,
    gv_ref,
    gt_ref,
    q_own,
    cot_own,
    k_all,
    v_all,
    q_next,
    grad_own,
    grad_next,
    gain_ref,
    table_ref,
    picks,
    ring_rows,
    bias,
    bias_turned,
    prob,
    lows,
    prob_next,
    att,
    sums,
    norms,
    stat_out,
    stat_in,
    own_k,
    own_v,
    marks,
    mark_out,
    mark_in,
    rowdots,
    tab_own,
    tab_out,
    tab_in,
    gain_row,
    load_sem,
    send_sem,
    recv_sem,
    mark_sem,
    stat_send,
    stat_recv,
    tab_send,
    tab_recv,
    met_sem,
):
    rows, width = q_own.shape
    heads = width // HEAD_DIM
    tiles = rows // ROWS
    cross = min(tiles, REACH // ROWS)
    rel = table_ref.shape[1]
    columns = picks.shape[1]
    stages = (sp_count - 2).bit_length()
    early = max(min(stages, heads - 2), 0)
    scale = 1.0 / math.sqrt(HEAD_DIM)
    sp_me, tp_me = lax.axis_index("sp"), lax.axis_index("tp")
    after = jnp.minimum(sp_me + 1, sp_count - 1)
    before = jnp.maximum(sp_me - 1, 0)
    has_after, has_before = sp_me < sp_count - 1, sp_me > 0
    has_both = has_after & has_before

    loads = [
        pltpu.make_async_copy(src, dst, load_sem.at[i])
        for i, (src, dst) in enumerate(
            (
                (k_hbm.at[0], k_all.at[pl.ds(REACH, rows), :]),
                (v_hbm.at[0], v_all.at[pl.ds(REACH, rows), :]),
                (q_hbm.at[0], q_own),
                (gain_hbm, gain_ref),
                (table_hbm, table_ref),
                (cot_hbm.at[0], cot_own),
            )
        )
    ]
    for load in loads:
        load.start()

    def cols(h):
        return pl.ds(pl.multiple_of(h * HEAD_DIM, HEAD_DIM), HEAD_DIM)

    def remote(src, dst, send, recv, axis, peer):
        return pltpu.make_async_remote_copy(
            src_ref=src,
            dst_ref=dst,
            send_sem=send,
            recv_sem=recv,
            device_id={axis: peer},
            device_id_type=pl.DeviceIdType.MESH,
        )

    def along(kind, h, src, dst, peer):
        return remote(src, dst, send_sem.at[kind, h], recv_sem.at[kind, h], "sp", peer)

    def forward_copies(h):
        last = pl.ds(rows, REACH)
        first = pl.ds(0, REACH)
        return (
            along(0, h, k_all.at[last, cols(h)], k_all.at[first, cols(h)], after),
            along(1, h, v_all.at[last, cols(h)], v_all.at[first, cols(h)], after),
        )

    def query_copy(h):
        return along(2, h, q_own.at[:, cols(h)], q_next.at[:, cols(h)], before)

    def grad_copy(h):
        return along(3, h, grad_own.at[h], grad_next.at[h], before)

    def mark_copy(i):
        return remote(mark_out.at[i], mark_in.at[i], mark_sem.at[0, i], mark_sem.at[1, i], "sp", before)

    def stat_copy(i):
        peer = lax.rem(tp_me + 1 + i, tp_count)
        return remote(stat_out, stat_in.at[i], stat_send.at[i], stat_recv.at[i], "tp", peer)

    def tab_copy(i):
        peer = lax.rem(sp_me + 1 + i, sp_count)
        return remote(tab_out, tab_in.at[i], tab_send.at[i], tab_recv.at[i], "sp", peer)

    def each(count, body):
        def step(i, carry):
            body(i)
            return carry

        lax.fori_loop(0, count, step, 0)

    def signal(semaphore, axis, peer):
        pl.semaphore_signal(
            semaphore, inc=1, device_id={axis: peer}, device_id_type=pl.DeviceIdType.MESH
        )

    def greet(semaphore, distance):
        right, left = sp_me + distance, sp_me - distance

        @pl.when(right < sp_count)
        def _():
            signal(semaphore, "sp", right)

        @pl.when(left >= 0)
        def _():
            signal(semaphore, "sp", left)

    def greeters(distance):
        right, left = sp_me + distance, sp_me - distance
        return (right < sp_count).astype(jnp.int32) + (left >= 0).astype(jnp.int32)

    def meet(stage):
        pl.semaphore_wait(met_sem.at[stage], greeters(1 << stage))
        if stage + 1 < stages:
            greet(met_sem.at[stage + 1], 1 << (stage + 1))

    barrier = pltpu.get_barrier_semaphore()
    pl.when(has_before)(lambda: signal(barrier, "sp", before))
    each(tp_count - 1, lambda i: signal(barrier, "tp", lax.rem(tp_me + 1 + i, tp_count)))
    for load in loads[:2]:
        load.wait()
    pl.semaphore_wait(barrier, has_after.astype(jnp.int32) + tp_count - 1)

    @pl.when(has_after)
    def _():
        def body(h):
            for copy in forward_copies(h):
                copy.start()

        each(heads, body)

    for load in loads[2:]:
        load.wait()

    def send_queries(which):
        for h in which:
            query_copy(h).start()


    @pl.when(jnp.logical_not(has_before))
    def _():
        k_all[:REACH, :] = jnp.zeros((REACH, width), BF16)
        v_all[:REACH, :] = jnp.zeros((REACH, width), BF16)

    gain_row[...] = gain_ref[...].astype(F32).reshape(1, width)
    picks[...] = distance_picks(rel, columns, 1, 7)
    table = jnp.concatenate([table_ref[...].astype(F32), jnp.zeros((8 - heads, rel), F32)], axis=0)
    ring_rows[...] = dot(table.astype(BF16), distance_picks(rel, columns, 0, 0)[:rel], 1, 0)
    query_seg = iota((ROWS, COLS), 0) // SEG
    key_seg = iota((ROWS, COLS), 1) // SEG
    in_band = (key_seg >= query_seg) & (key_seg <= query_seg + LEFT)

    def bias_of(h):
        spread = spread_rows(ring_rows[pl.ds(h, 1), :])[:, :COLS]
        banded = jnp.where(in_band, spread, masked_value)
        bias[h] = banded
        bias_turned[h] = banded[:, :REACH].T

    each(heads, bias_of)
    sums[...] = jnp.zeros_like(sums)
    marks[...] = jnp.zeros_like(marks)
    mark_lane = iota((rows, HEAD_DIM), 1)

    def forward(h):
        @pl.when(has_before)
        def _():
            for copy in forward_copies(h):
                copy.wait_recv()

        @pl.when(has_both)
        def _():
            for copy in forward_copies(h):
                copy.wait_send()

        for step, which in QUERY_STARTS(heads).items():
            pl.when(has_both & (h == step))(functools.partial(send_queries, which))
        pl.when(has_before & jnp.logical_not(has_after) & (h == 0))(lambda: send_queries(range(heads)))
        if stages:
            pl.when(h == 0)(lambda: greet(met_sem.at[0], 1))
        for stage in range(early):
            pl.when(h == stage + 1)(functools.partial(meet, stage))

        gain = gain_row[:, cols(h)]
        levels = []
        for b in range(tiles):
            here = slice(b * ROWS, (b + 1) * ROWS)
            band = slice(b * ROWS, b * ROWS + COLS)
            scores = dot(q_own[here, cols(h)], k_all[band, cols(h)], 1, 1) * scale + bias[h]
            first_key = (sp_me * rows) - REACH + b * ROWS
            scores = jnp.where(iota((1, COLS), 1) + first_key >= 0, scores, masked_value)
            row_max = jnp.max(scores, axis=1, keepdims=True)
            shifted = jnp.exp(scores - row_max)
            row_total = jnp.sum(shifted, axis=1, keepdims=True)
            p = shifted * (1.0 / row_total)
            levels.append(row_max + jnp.log(row_total))
            prob[h, b] = p
            attended = dot(p.astype(BF16), v_all[band, cols(h)], 1, 0)
            att[here, cols(h)] = attended
            scaled = cot_own[here, cols(h)].astype(F32) * gain
            sums[0, here, :] += attended * attended
            sums[1, here, :] += attended * scaled
        marks[...] = jnp.where(mark_lane == h, jnp.concatenate(levels, axis=0), marks[...])

    each(heads, forward)

    lane = iota((rows, HEAD_DIM), 1)
    squares = jnp.sum(sums[0], axis=1, keepdims=True)
    products = jnp.sum(sums[1], axis=1, keepdims=True)
    packed = jnp.where(lane == 0, squares, jnp.where(lane == 1, products, 0.0))
    stat_out[...] = packed.T[:2]
    each(tp_count - 1, lambda i: stat_copy(i).start())
    mark_out[0] = marks[...].T[: mark_out.shape[1]]
    pl.when(has_before)(lambda: mark_copy(0).start())

    total = stat_out[...]
    for i in range(tp_count - 1):
        stat_copy(i).wait_recv()
        total = total + stat_in[i]
    total = total * (1.0 / (width * tp_count))
    whole = jnp.concatenate([total, jnp.zeros((HEAD_DIM - 2, rows), F32)], axis=0).T
    inv_rms = lax.rsqrt(whole[:, 0:1] + epsilon)
    norms[0] = jnp.broadcast_to(inv_rms, (rows, HEAD_DIM))
    norms[1] = jnp.broadcast_to(inv_rms * inv_rms * inv_rms * whole[:, 1:2], (rows, HEAD_DIM))

    row_marks = jnp.zeros((rows, HEAD_DIM), F32)
    for h in range(heads):
        here = slice(h * HEAD_DIM, (h + 1) * HEAD_DIM)
        scaled = cot_own[:, here].astype(F32) * gain_row[:, here]
        attended = att[:, here]
        grad = (norms[0] * scaled - attended * norms[1]).astype(BF16)
        grad_own[h] = grad
        if h == 0:
            pl.when(has_before)(lambda: grad_copy(0).start())
        row_dot = jnp.sum(grad.astype(F32) * attended, axis=1, keepdims=True)
        rowdots[h] = jnp.broadcast_to(row_dot, (rows, HEAD_DIM))
        row_marks = jnp.where(mark_lane == h, row_dot, row_marks)
    mark_out[1] = row_marks.T[: mark_out.shape[1]]

    @pl.when(has_before)
    def _():
        mark_copy(1).start()
        for h in range(1, min(2, heads)):
            grad_copy(h).start()

    def score_grads(h):
        folded = None
        for b in range(tiles):
            here = slice(b * ROWS, (b + 1) * ROWS)
            band = slice(b * ROWS, b * ROWS + COLS)
            across = slice(h * HEAD_DIM, (h + 1) * HEAD_DIM)
            grad_p = dot(grad_own[h, here], v_all[band, across], 1, 1)
            row_dot = jnp.concatenate([rowdots[h, here]] * (COLS // HEAD_DIM), axis=1)
            grad_s = prob[h, b] * (grad_p - row_dot)
            lows[h, b] = grad_s.astype(BF16)
            folded = grad_s if folded is None else folded + grad_s
        return jnp.concatenate([folded, jnp.zeros((ROWS, ROLL - COLS), F32)], axis=1)

    def backward(h):
        for b in range(tiles):
            here = slice(b * ROWS, (b + 1) * ROWS)
            band = slice(b * ROWS, b * ROWS + COLS)
            gq_ref[0, here, cols(h)] = (dot(lows[h, b], k_all[band, cols(h)], 1, 0) * scale).astype(BF16)
        for t in range(tiles):
            mine = slice(t * ROWS, (t + 1) * ROWS)
            key_sum, value_sum = None, None
            for b in range(tiles):
                begin = REACH + (t - b) * ROWS
                if not 0 <= begin < COLS:
                    continue
                here = slice(b * ROWS, (b + 1) * ROWS)
                piece = slice(begin, begin + ROWS)
                key_part = dot(lows[h, b, :, piece], q_own[here, cols(h)], 0, 0)
                value_part = dot(prob[h, b, :, piece].astype(BF16), grad_own[h, here], 0, 0)
                key_sum = key_part if key_sum is None else key_sum + key_part
                value_sum = value_part if value_sum is None else value_sum + value_part
            own_k[h, mine] = key_sum
            own_v[h, mine] = value_sum

    rings = [fold_rows(score_grads(h)) for h in range(heads)]
    rings = jnp.concatenate(rings + [jnp.zeros((8 - heads, ROLL), F32)], axis=0)
    parts = dot(in_parts(rings), picks[...], 1, 0)
    parts = (parts[:8] + parts[8:16] + parts[16:])[:heads]
    lines = [parts[:, i : i + HEAD_DIM] for i in range(0, columns, HEAD_DIM)]
    if tab_own.shape[0] > heads * len(lines):
        lines.append(jnp.zeros((tab_own.shape[0] - heads * len(lines), HEAD_DIM), F32))
    tab_own[...] = jnp.concatenate(lines, axis=0)
    tab_out[...] = tab_own[...].astype(BF16)
    for stage in range(early, stages):
        meet(stage)
    each(sp_count - 1, lambda i: tab_copy(i).start())

    @pl.when(has_before)
    def _():
        for h in range(min(2, heads), heads):
            grad_copy(h).start()

    def next_probs(h):
        query_copy(h).wait_recv()
        for b in range(cross):
            here = slice(b * ROWS, (b + 1) * ROWS)
            mine = slice(rows + b * ROWS, rows + REACH)
            count = REACH - b * ROWS
            scores = dot(k_all[mine, cols(h)], q_next[here, cols(h)], 1, 1) * scale
            level = mark_in[0, pl.ds(h, 1), :][:, here]
            prob_next[h, b, :count] = jnp.exp(scores + bias_turned[h, :count] - level)

    @pl.when(has_after)
    def _():
        mark_copy(0).wait_recv()
        each(heads, next_probs)

    each(heads, backward)
    pl.when(has_after)(lambda: mark_copy(1).wait_recv())

    def finish(h):
        @pl.when(has_after)
        def _():
            grad_copy(h).wait_recv()
            for b in range(cross):
                here = slice(b * ROWS, (b + 1) * ROWS)
                mine = slice(rows + b * ROWS, rows + REACH)
                out = slice(rows - REACH + b * ROWS, rows)
                count = REACH - b * ROWS
                grad = grad_next[h, here]
                p = prob_next[h, b, :count]
                grad_p = dot(v_all[mine, cols(h)], grad, 1, 1)
                low = (p * (grad_p - mark_in[1, pl.ds(h, 1), :][:, here])).astype(BF16)
                own_k[h, out] += dot(low, q_next[here, cols(h)], 1, 0)
                own_v[h, out] += dot(p.astype(BF16), grad, 1, 0)

        gv_ref[0, :, cols(h)] = own_v[h].astype(BF16)
        gk_ref[0, :, cols(h)] = (own_k[h] * scale).astype(BF16)

    each(heads - 1, finish)

    def receive_table(i, total):
        tab_copy(i).wait_recv()
        return total + tab_in[i].astype(F32)

    total = lax.fori_loop(0, sp_count - 1, receive_table, tab_own[...])
    lines = [total[i * heads : (i + 1) * heads] for i in range(columns // HEAD_DIM)]
    gt_ref[...] = jnp.concatenate(lines, axis=1)[:, :rel]

    @pl.when(has_before)
    def _():
        def body(h):
            query_copy(h).wait_send()
            grad_copy(h).wait_send()

        each(heads, body)
        for i in range(2):
            mark_copy(i).wait_send()

    @pl.when(has_after & jnp.logical_not(has_before))
    def _():
        def body(h):
            for copy in forward_copies(h):
                copy.wait_send()

        each(heads, body)

    each(tp_count - 1, lambda i: stat_copy(i).wait_send())
    each(sp_count - 1, lambda i: tab_copy(i).wait_send())
    finish(heads - 1)


def QUERY_STARTS(heads):
    return {heads - 2: [0], heads - 1: range(1, heads)}


def put_out(*refs):
    count = (len(refs) - 1) // 2
    sources, targets, sem = refs[:count], refs[count : 2 * count], refs[-1]
    stores = [pltpu.make_async_copy(sources[i], targets[i], sem.at[i]) for i in range(count)]
    for store in stores:
        store.start()
    for store in stores:
        store.wait()


def on_device(sp_count, tp_count, queries, key_vectors, value_vectors, cotangent, out_gain, table):
    _, rows, width = queries.shape
    heads = width // HEAD_DIM
    rel = table.shape[1]
    tiles = rows // ROWS
    cross = min(tiles, REACH // ROWS)
    span = REACH + rows
    dma = pltpu.SemaphoreType.DMA
    vmem = pl.BlockSpec(memory_space=pltpu.VMEM)
    far = pl.BlockSpec(memory_space=pltpu.HBM)
    columns = -(-rel // HEAD_DIM) * HEAD_DIM
    marks = -(-heads // 8) * 8
    lines = -(-heads * columns // HEAD_DIM // 16) * 16
    stages = max((sp_count - 2).bit_length(), 1)
    shapes = (
        jax.ShapeDtypeStruct(queries.shape, BF16),
        jax.ShapeDtypeStruct(queries.shape, BF16),
        jax.ShapeDtypeStruct(queries.shape, BF16),
        jax.ShapeDtypeStruct((heads, rel), F32),
    )
    grads = pl.pallas_call(
        functools.partial(kernel, sp_count, tp_count),
        out_shape=tuple(pltpu.VMEM(shape.shape, shape.dtype) for shape in shapes),
        in_specs=[far] * 6,
        out_specs=(vmem,) * 4,
        scratch_shapes=[
            pltpu.VMEM((rows, width), BF16),
            pltpu.VMEM((rows, width), BF16),
            pltpu.VMEM((span, width), BF16),
            pltpu.VMEM((span, width), BF16),
            pltpu.VMEM((rows, width), BF16),
            pltpu.VMEM((heads, rows, HEAD_DIM), BF16),
            pltpu.VMEM((heads, rows, HEAD_DIM), BF16),
            pltpu.VMEM((width,), BF16),
            pltpu.VMEM((heads, rel), BF16),
            pltpu.VMEM((ROLL, columns), BF16),
            pltpu.VMEM((8, ROLL), F32),
            pltpu.VMEM((heads, ROWS, COLS), F32),
            pltpu.VMEM((heads, REACH, ROWS), F32),
            pltpu.VMEM((heads, tiles, ROWS, COLS), F32),
            pltpu.VMEM((heads, tiles, ROWS, COLS), BF16),
            pltpu.VMEM((heads, cross, REACH, ROWS), F32),
            pltpu.VMEM((rows, width), F32),
            pltpu.VMEM((2, rows, HEAD_DIM), F32),
            pltpu.VMEM((2, rows, HEAD_DIM), F32),
            pltpu.VMEM((2, rows), F32),
            pltpu.VMEM((tp_count - 1, 2, rows), F32),
            pltpu.VMEM((heads, rows, HEAD_DIM), F32),
            pltpu.VMEM((heads, rows, HEAD_DIM), F32),
            pltpu.VMEM((rows, HEAD_DIM), F32),
            pltpu.VMEM((2, marks, rows), F32),
            pltpu.VMEM((2, marks, rows), F32),
            pltpu.VMEM((heads, rows, HEAD_DIM), F32),
            pltpu.VMEM((lines, HEAD_DIM), F32),
            pltpu.VMEM((lines, HEAD_DIM), BF16),
            pltpu.VMEM((sp_count - 1, lines, HEAD_DIM), BF16),
            pltpu.VMEM((1, width), F32),
            dma((6,)),
            dma((4, heads)),
            dma((4, heads)),
            dma((2, 2)),
            dma((tp_count - 1,)),
            dma((tp_count - 1,)),
            dma((sp_count - 1,)),
            dma((sp_count - 1,)),
            pltpu.SemaphoreType.REGULAR((stages,)),
        ],
        compiler_params=pltpu.CompilerParams(
            collective_id=0, has_side_effects=True, vmem_limit_bytes=60 * 1024 * 1024
        ),
        name="segment_attention_backward",
    )(queries, key_vectors, value_vectors, cotangent, out_gain, table)
    return pl.pallas_call(
        put_out,
        out_shape=shapes,
        in_specs=[vmem] * 4,
        out_specs=(far,) * 4,
        scratch_shapes=[dma((4,))],
        compiler_params=pltpu.CompilerParams(vmem_limit_bytes=1024 * 1024),
        name="put_out",
    )(*grads)


def solution(mesh):
    return jax.shard_map(
        functools.partial(on_device, mesh.shape["sp"], mesh.shape["tp"]),
        mesh=mesh,
        in_specs=(
            P(None, "sp", "tp"),
            P(None, "sp", "tp"),
            P(None, "sp", "tp"),
            P(None, "sp", "tp"),
            P("tp"),
            P("tp", None),
        ),
        out_specs=(P(None, "sp", "tp"), P(None, "sp", "tp"), P(None, "sp", "tp"), P("tp", None)),
        check_vma=False,
    )
```
